128 devices in a mesh: ep: 32 (over z, y, core), tp: 4 (over x).
Axes of the slice: x: 4, y: 4, z: 4, core: 2. Of those that a mesh axis runs over, the one named last changes fastest.
Arguments:
- query_rows: bfloat16 [32768, 1024], P('ep', 'tp'), may hold values from -140 to 140
- key_rows: bfloat16 [32768, 256], P('ep', 'tp'), may hold values from -4.5 to 4.5
- value_rows: bfloat16 [32768, 256], P('ep', 'tp'), may hold values from -6 to 6
- sink_logit: float32 [16], P('tp'), may hold values from 1 to 6
- out_weight: bfloat16 [1024, 2048], P('tp'), may hold values from -0.1875 to 0.1875
- routed_rows: bfloat16 [16384, 2048], P(('ep', 'tp')), may hold values from -6 to 6
- norm_gain: float32 [2048], replicated, may hold values from 0.1 to 1.9
- routing: int32 [16384, 2], P(('ep', 'tp')), may hold values from 0 to 31, all different within a row; in each aligned block of 128 rows (0 to 127, 128 to 255, ...) at most 9 rows name the same one
- route_weight: float32 [16384, 2], P(('ep', 'tp')), may hold values from 0.2 to 1
- gate_weight: bfloat16 [32, 2048, 7168], P('ep', None, 'tp'), may hold values from -0.125 to 0.125
- up_weight: bfloat16 [32, 2048, 7168], P('ep', None, 'tp'), may hold values from -0.125 to 0.125
- down_weight: bfloat16 [32, 7168, 2048], P('ep', 'tp'), may hold values from -0.0625 to 0.0625
Outputs:
- mixed_rows: bfloat16 [32768, 2048], P(('ep', 'tp'))
- expert_mix: bfloat16 [16384, 2048], P(('ep', 'tp'))
The draws below stay inside these ranges and needn't reach their ends.
Inputs may be any that keep to these rules, and one draw needn't show every extreme that they name: `routing`: each token names 2 different experts. Within the 128 rows of one device no expert is named by more than 9 rows, and in every draw some device's rows name some expert exactly 9 times.
All inputs are finite; a program needn't handle non-finite values.
Results may differ from the reference program's by a relative error of at most 0.012.
Values may be sent and summed in bfloat16 or wider, within the bound.
No kernel may reach another device: no remote copies, remote signals or barrier semaphores. Data moves between devices by JAX's collectives and lax.ppermute only.
A program may use at most 128 MiB of HBM per device.

```python
import math
import jax
import jax.numpy as jnp
import numpy as np
from jax import lax

D = 2048
HEADS = 16
KV_HEADS = 4
HEAD_DIM = 64
WINDOW = 128
FF = 7168
TOP = 2
MOE_DEV = 128
SEQ = 32768
TOKENS = 16384
EXPERTS = 32
CAP = 9
N_EP = 32
N_TP = 4


def base_pair(key):
    query_base = jnp.clip(jax.random.normal(jax.random.fold_in(key, 11), (SEQ, HEADS * HEAD_DIM), jnp.float32), -4.5, 4.5)
    key_base = jnp.clip(jax.random.normal(jax.random.fold_in(key, 12), (SEQ, KV_HEADS * HEAD_DIM), jnp.float32), -4.5, 4.5)
    return (query_base, key_base)


def draw_query_rows(key, part):
    query_base, key_base = base_pair(key)
    return query_base.astype(jnp.bfloat16)


def draw_key_rows(key, part):
    query_base, key_base = base_pair(key)
    return key_base.astype(jnp.bfloat16)


def levels(own_key, dims, shards, low, largest):
    gain = 1.0
    for position, shards_of in shards:
        heights = jax.random.uniform(jax.random.fold_in(jax.random.fold_in(own_key, 6), position), (shards_of,), jnp.float32, low / len(shards), largest / len(shards))
        gain = gain * jnp.repeat(jnp.exp(heights), dims[position] // shards_of).reshape((-1,) + (1,) * (len(dims) - 1 - position))
    return gain


def shared_out(key, own, number, rows, amount, top, most, slope):
    ranking = jax.random.permutation(key, amount)
    crowded, common = portions_of(amount, rows * top, most, slope, True), portions_of(amount, rows * top, most, slope, False)
    places = jnp.arange(amount)

    def named(lengths, rotation):
        used = int((lengths > 0).sum())
        fixed = max(1, used // 4)
        passed = fixed + (places - fixed + rotation * (used - fixed)) % max(1, amount - fixed)
        return jnp.zeros((amount,), jnp.int32).at[ranking[jnp.where(places < fixed, places, passed)]].set(jnp.asarray(lengths, jnp.int32))

    lengths = jnp.where(number % 4 == 0, named(crowded, number // 4), named(common, number - number // 4 - 1))
    mixed = jax.random.permutation(jax.random.fold_in(own, 3), amount)
    source_of, receiver = mixed[0:amount // 2 * 2:2], mixed[1:amount // 2 * 2:2]
    margin = jnp.minimum(lengths[source_of] - 1, most - lengths[receiver]) // 2
    margin = jnp.where((source_of == ranking[0]) | (receiver == ranking[0]) | (lengths[receiver] == 0), 0, jnp.maximum(margin, 0))
    passed = jax.random.randint(jax.random.fold_in(own, 4), (amount // 2,), 0, 1 << 20) % (margin + 1)
    lengths = lengths.at[source_of].add(-passed).at[receiver].add(passed)
    items = jnp.searchsorted(jnp.cumsum(lengths), jnp.arange(rows * top), side="right").astype(jnp.int32)
    table = items.reshape(top, rows).T
    table = table[jax.random.permutation(jax.random.fold_in(own, 1), rows)]
    rotation = jax.random.randint(jax.random.fold_in(own, 2), (rows, 1), 0, top)
    return jnp.take_along_axis(table, (jnp.arange(top)[None, :] + rotation) % top, axis=1)


def portions_of(number_of, total, most, skew, full):
    weights = [(1 << 20) // math.isqrt(standing ** skew) + 1 for standing in range(1, number_of + 1)]
    largest = most if full else min(most, max(-(-total // number_of), total * weights[0] // sum(weights)))
    least = 1 if total - largest >= number_of - 1 else 0
    counts, rest = [largest] + [least] * (number_of - 1), total - largest - least * (number_of - 1)
    while rest > 0:
        free = [i for i in range(1, number_of) if counts[i] < largest] or [i for i in range(1, number_of) if counts[i] < most]
        pool, left = sum([weights[i] for i in free]), rest
        for i in free:
            addition = min(most - counts[i], max(1, left * weights[i] // pool), rest)
            counts[i] = counts[i] + addition
            rest = rest - addition
    return np.array(counts)


def noise(own_key, extent, spread, bound, split=(), kind=jnp.bfloat16):
    entries = jax.random.normal(own_key, extent, jnp.float32) * spread
    if len(split) > 0:
        entries = levels(own_key, extent, split, -0.22, 0.18) * entries
    return jnp.clip(entries, min=-bound, max=bound).astype(kind)


def setup_inputs(seed: int = 0) -> dict:
    key_list = jax.random.split(jax.random.key(seed), 13)
    query_rows = draw_query_rows(jax.random.fold_in(key_list[12], 71), 0)
    key_rows = draw_key_rows(jax.random.fold_in(key_list[12], 71), 0)
    value_rows = noise(key_list[2], (SEQ, KV_HEADS * HEAD_DIM), 1.0, 6.0, ((0, 32), (1, 4)))
    sink_logit = jnp.clip(1.0 + 5.0 * jax.random.uniform(key_list[3], (HEADS,), jnp.float32) ** levels(key_list[3], (HEADS,), ((0, 4),), -0.2, 0.2), 1.0, 6.0)
    out_weight = noise(key_list[4], (HEADS * HEAD_DIM, D), (HEADS * HEAD_DIM) ** -0.5, 0.1875, ((0, 4),))
    routed_rows = noise(key_list[5], (TOKENS, D), 1.0, 6.0, ((0, 128),))
    norm_gain = jnp.clip(1.0 + 0.18 * jax.random.normal(key_list[6], (D,), jnp.float32), 0.1, 1.9)
    routing_keys = jax.random.split(jax.random.fold_in(key_list[7], 1), TOKENS // MOE_DEV)
    routing_turns = jax.random.permutation(jax.random.fold_in(key_list[7], 3), TOKENS // MOE_DEV)
    routing = jax.vmap(lambda own, number: shared_out(jax.random.fold_in(key_list[7], 2), own, number, MOE_DEV, EXPERTS, TOP, CAP, 0))(routing_keys, routing_turns).reshape((TOKENS, TOP))
    route_weight = jnp.clip(0.2 + 0.8 * jax.random.uniform(key_list[8], (TOKENS, TOP), jnp.float32) ** levels(key_list[8], (TOKENS, TOP), ((0, 128),), -0.2, 0.2), 0.2, 1.0)
    gate_weight = noise(key_list[9], (EXPERTS, D, FF), D ** -0.5, 0.125, ((0, 32), (2, 4)))
    up_weight = noise(key_list[10], (EXPERTS, D, FF), D ** -0.5, 0.125, ((0, 32), (2, 4)))
    down_weight = noise(key_list[11], (EXPERTS, FF, D), FF ** -0.5, 0.0625, ((0, 32), (1, 4)))
    return {"query_rows": query_rows, "key_rows": key_rows, "value_rows": value_rows, "sink_logit": sink_logit, "out_weight": out_weight, "routed_rows": routed_rows, "norm_gain": norm_gain, "routing": routing, "route_weight": route_weight, "gate_weight": gate_weight, "up_weight": up_weight, "down_weight": down_weight}


EPS = 1e-06

def attention_part(query_rows, key_rows, value_rows, sink_logit):
    seq_total = query_rows.shape[0]
    group_size = HEADS // KV_HEADS
    block_rows = min(512, seq_total)
    score_scale = HEAD_DIM ** (-0.5)
    key_pad = jnp.pad(key_rows.astype(jnp.float32), ((WINDOW, WINDOW), (0, 0)))
    value_pad = jnp.pad(value_rows.astype(jnp.float32), ((WINDOW, WINDOW), (0, 0)))
    query_all = query_rows.astype(jnp.float32)
    sink_col = sink_logit.astype(jnp.float32).reshape(KV_HEADS, group_size)[:, :, None]

    def one_block(block_index):
        first_row = block_index * block_rows
        query_block = lax.dynamic_slice_in_dim(query_all, first_row, block_rows, 0).reshape(block_rows, KV_HEADS, group_size, HEAD_DIM)
        key_block = lax.dynamic_slice_in_dim(key_pad, first_row, block_rows + 2 * WINDOW, 0).reshape(-1, KV_HEADS, HEAD_DIM)
        value_block = lax.dynamic_slice_in_dim(value_pad, first_row, block_rows + 2 * WINDOW, 0).reshape(-1, KV_HEADS, HEAD_DIM)
        scores = jnp.einsum('qkgd,skd->kgqs', query_block, key_block) * score_scale
        query_pos = first_row + jnp.arange(block_rows, dtype=jnp.int32)
        key_pos = first_row - WINDOW + jnp.arange(block_rows + 2 * WINDOW, dtype=jnp.int32)
        inside = (jnp.abs(key_pos[None, :] - query_pos[:, None]) <= WINDOW) & (key_pos >= 0)[None, :] & (key_pos < seq_total)[None, :]
        scores = jnp.where(inside, scores, -jnp.inf)
        row_peak = jnp.maximum(lax.optimization_barrier(jnp.max(scores, axis=-1)), sink_col)
        weights = jnp.where(inside, jnp.exp(scores - row_peak[..., None]), 0.0)
        total_weight = lax.optimization_barrier(jnp.sum(weights, axis=-1)) + jnp.exp(sink_col - row_peak)
        rounded = lax.optimization_barrier(weights.astype(jnp.bfloat16)).astype(jnp.float32)
        attended = jnp.einsum('kgqs,skd->qkgd', rounded, value_block) / jnp.transpose(total_weight, (2, 0, 1))[..., None]
        return attended.reshape(block_rows, HEADS * HEAD_DIM).astype(jnp.bfloat16)
    pieces = lax.map(one_block, jnp.arange(seq_total // block_rows, dtype=jnp.int32))
    return pieces.reshape(seq_total, HEADS * HEAD_DIM)

def expert_part(routed_rows, norm_gain, routing, route_weight, gate_weight, up_weight, down_weight):
    token_count = routed_rows.shape[0]
    values = routed_rows.astype(jnp.float32)
    normed = (values * lax.rsqrt(lax.optimization_barrier(jnp.mean(values * values, axis=-1, keepdims=True)) + EPS) * norm_gain.astype(jnp.float32)).astype(jnp.bfloat16)
    slot_limit = N_EP * N_TP * CAP
    shard_width = FF // N_TP

    def per_expert(carry, stacked):
        expert_id, gate_one, up_one, down_one = stacked
        chosen = routing == expert_id
        weight_one = lax.optimization_barrier(jnp.sum(jnp.where(chosen, route_weight.astype(jnp.float32), 0.0), axis=1))
        is_routed = jnp.any(chosen, axis=1)
        slot_place = (jnp.cumsum(is_routed.astype(jnp.int32)) - 1).astype(jnp.int32)
        slot_place = jnp.where(is_routed, slot_place, slot_limit).astype(jnp.int32)
        slot_row = jnp.zeros((slot_limit,), jnp.int32).at[slot_place].set(jnp.arange(token_count, dtype=jnp.int32), mode='drop')
        filled = jnp.arange(slot_limit, dtype=jnp.int32) < jnp.sum(is_routed.astype(jnp.int32))
        gathered = normed[slot_row].astype(jnp.float32)
        gate_pre = jnp.dot(gathered, gate_one.astype(jnp.float32), preferred_element_type=jnp.float32)
        up_pre = jnp.dot(gathered, up_one.astype(jnp.float32), preferred_element_type=jnp.float32)
        hidden = (jax.nn.silu(gate_pre) * up_pre).astype(jnp.bfloat16).astype(jnp.float32)
        summed = jnp.zeros((slot_limit, D), jnp.float32)
        for shard_index in range(N_TP):
            low = shard_index * shard_width
            part_rows = jnp.dot(hidden[:, low:low + shard_width], down_one[low:low + shard_width].astype(jnp.float32), preferred_element_type=jnp.float32)
            summed = summed + lax.optimization_barrier(part_rows.astype(jnp.bfloat16)).astype(jnp.float32)
        scaled = summed * jnp.where(filled, weight_one[slot_row], 0.0)[:, None]
        return (carry.at[slot_row].add(scaled), None)
    mixed_sum, unused = lax.scan(per_expert, jnp.zeros((token_count, D), jnp.float32), (jnp.arange(EXPERTS, dtype=jnp.int32), gate_weight, up_weight, down_weight))
    return mixed_sum.astype(jnp.bfloat16)

def reference(query_rows, key_rows, value_rows, sink_logit, out_weight, routed_rows, norm_gain, routing, route_weight, gate_weight, up_weight, down_weight):
    attended = attention_part(query_rows, key_rows, value_rows, sink_logit)
    mixed_rows = jnp.dot(attended.astype(jnp.float32), out_weight.astype(jnp.float32), preferred_element_type=jnp.float32).astype(jnp.bfloat16)
    expert_mix = expert_part(routed_rows, norm_gain, routing, route_weight, gate_weight, up_weight, down_weight)
    return (mixed_rows, expert_mix)
```

```python
import functools

import jax
import jax.numpy as jnp
from jax import lax
from jax.experimental import pallas as pl
from jax.experimental.pallas import tpu as pltpu
from jax.sharding import PartitionSpec as P


HEAD_DIM = 64
WINDOW = 128
EPS = 1e-06
CAP = 9
MAIN = 8
F32 = jnp.float32
BF16 = jnp.bfloat16


def dot(a, b, dims=((1,), (0,))):
    return lax.dot_general(a, b, (dims, ((), ())), preferred_element_type=F32)


def slot_iota(shape, experts):
    slot = lax.broadcasted_iota(jnp.int32, shape, 0)
    main = slot < experts * MAIN
    expert_of = jnp.where(main, lax.shift_right_logical(slot, 3), slot - experts * MAIN)
    return expert_of, jnp.where(main, slot & (MAIN - 1), MAIN)


def dispatch_kernel(rows_ref, gain_ref, routing_ref, weight_ref, out_ref, high_ref, low_ref, *, experts):
    tokens, width = rows_ref.shape
    x = rows_ref[...].astype(F32)
    mean = jnp.mean(x * x, axis=-1, keepdims=True)
    normed = (x * lax.rsqrt(mean + EPS) * gain_ref[...]).astype(BF16)
    ids = lax.broadcasted_iota(jnp.int32, (experts, tokens), 0)
    hot0 = routing_ref[0:1, :] == ids
    hot1 = routing_ref[1:2, :] == ids
    member = jnp.where(hot0 | hot1, 1.0, 0.0)
    row = lax.broadcasted_iota(jnp.int32, (tokens, tokens), 0)
    col = lax.broadcasted_iota(jnp.int32, (tokens, tokens), 1)
    upper = jnp.where(row <= col, 1.0, 0.0).astype(BF16)
    place = (dot(member.astype(BF16), upper) * member).astype(BF16)
    gate = jnp.where(hot0, weight_ref[0:1, :], 0.0) + jnp.where(hot1, weight_ref[1:2, :], 0.0)
    high = gate.astype(BF16)
    low = (gate - high.astype(F32)).astype(BF16)
    slots = experts * CAP
    expert_of, _ = slot_iota((slots, experts), experts)
    pick = jnp.where(expert_of == lax.broadcasted_iota(jnp.int32, (slots, experts), 1), 1.0, 0.0)
    pick = pick.astype(BF16)
    _, place_of = slot_iota((slots, tokens), experts)
    here = dot(pick, place) == (place_of + 1).astype(F32)
    high_ref[...] = jnp.where(here, dot(pick, high), 0.0).astype(BF16)
    low_ref[...] = jnp.where(here, dot(pick, low), 0.0).astype(BF16)
    rows = dot(jnp.where(here, 1.0, 0.0).astype(BF16), normed)
    last = []
    for j in range(width // 128):
        part = rows[:, j * 128 : (j + 1) * 128]
        tile = part[: experts * MAIN].reshape(experts, MAIN, 128).astype(BF16)
        out_ref[:, j * MAIN : (j + 1) * MAIN, :] = tile
        last.append(part[experts * MAIN :])
    out_ref[:, width // 128 * MAIN :, :] = jnp.stack(last, axis=1).astype(BF16)


def dispatch(routed_rows, norm_gain, routing, route_weight, experts):
    tokens, width = routed_rows.shape
    slots = experts * CAP
    matrix = jax.ShapeDtypeStruct((slots, tokens), BF16)
    return pl.pallas_call(
        functools.partial(dispatch_kernel, experts=experts),
        out_shape=(jax.ShapeDtypeStruct((experts, CAP * width // 128, 128), BF16), matrix, matrix),
        name="dispatch",
        cost_estimate=pl.CostEstimate(flops=400_000_000, transcendentals=0, bytes_accessed=2_500_000),
    )(routed_rows, norm_gain.reshape(1, width), routing.T, route_weight.T)


def attention_kernel(edge_ref, sink_ref, query_ref, kv_ref, vk_ref, out_ref):
    block = pl.program_id(0)
    size = WINDOW
    start = pl.multiple_of(block * size, size)
    kv = kv_ref[pl.ds(start, 3 * size), :]
    vk = vk_ref[pl.ds(start, 3 * size), :]
    lane = lax.broadcasted_iota(jnp.int32, (3 * size, 2 * HEAD_DIM), 1)
    left = lane < HEAD_DIM
    zero = jnp.zeros_like(kv)
    keys = jnp.concatenate([jnp.where(left, kv, zero), jnp.where(left, zero, vk)], axis=0)
    one = jnp.ones_like(kv)
    values = jnp.concatenate(
        [
            jnp.concatenate([jnp.where(left, vk, zero), jnp.where(left, one, zero)], axis=1),
            jnp.concatenate([jnp.where(left, zero, kv), jnp.where(left, zero, one)], axis=1),
        ],
        axis=0,
    )
    row = lax.broadcasted_iota(jnp.int32, (size, size), 0)
    col = lax.broadcasted_iota(jnp.int32, (size, size), 1)
    off_left = jnp.where((block == 0) & (edge_ref[0] == 1), 4 * size, 0)
    last = pl.num_programs(0) - 1
    off_right = jnp.where((block == last) & (edge_ref[1] == 1), 4 * size, 0)
    keep_left = col >= row + off_left
    keep_right = col + off_right <= row
    for pair in range(query_ref.shape[1] // (2 * HEAD_DIM)):
        lanes = slice(pair * 2 * HEAD_DIM, (pair + 1) * 2 * HEAD_DIM)
        query = query_ref[:, lanes] * jnp.asarray(HEAD_DIM**-0.5, BF16)
        scores = dot(query, keys, ((1,), (1,)))
        weights, sinks = [], []
        for one_head in range(2):
            low = one_head * 3 * size
            s0 = jnp.where(keep_left, scores[:, low : low + size], -jnp.inf)
            s1 = scores[:, low + size : low + 2 * size]
            s2 = jnp.where(keep_right, scores[:, low + 2 * size : low + 3 * size], -jnp.inf)
            sink = sink_ref[2 * pair + one_head]
            peak = jnp.max(jnp.maximum(jnp.maximum(s0, s1), s2), axis=1, keepdims=True)
            peak = jnp.maximum(peak, sink)
            weights += [jnp.exp(s - peak).astype(BF16) for s in (s0, s1, s2)]
            sinks.append(jnp.exp(sink - peak))
        total = dot(jnp.concatenate(weights, axis=1), values)
        lane_q = lax.broadcasted_iota(jnp.int32, (size, 2 * HEAD_DIM), 1)
        denominator = total[:, 2 * HEAD_DIM :] + jnp.where(lane_q < HEAD_DIM, sinks[0], sinks[1])
        out_ref[:, lanes] = (total[:, : 2 * HEAD_DIM] / denominator).astype(BF16)


def attention(query_rows, key_rows, value_rows, sink_logit):
    peers = lax.axis_size("ep")
    me = lax.axis_index("ep")
    up = [(i, i + 1) for i in range(peers - 1)]
    down = [(j, i) for i, j in up]
    joined = jnp.concatenate([key_rows, value_rows], axis=1)
    rows = joined.shape[0]
    before = lax.ppermute(joined[rows - WINDOW :], "ep", up)
    after = lax.ppermute(joined[:WINDOW], "ep", down)
    kv = jnp.concatenate([before, joined, after], axis=0)
    vk = jnp.concatenate([kv[:, HEAD_DIM:], kv[:, :HEAD_DIM]], axis=1)
    edge = jnp.stack([me == 0, me == peers - 1]).astype(jnp.int32)
    width = query_rows.shape[1]
    whole = lambda i: (0, 0)
    return pl.pallas_call(
        attention_kernel,
        grid=(rows // WINDOW,),
        in_specs=[
            pl.BlockSpec(memory_space=pltpu.SMEM),
            pl.BlockSpec(memory_space=pltpu.SMEM),
            pl.BlockSpec((WINDOW, width), lambda i: (i, 0)),
            pl.BlockSpec(kv.shape, whole),
            pl.BlockSpec(vk.shape, whole),
        ],
        out_specs=pl.BlockSpec((WINDOW, width), lambda i: (i, 0)),
        out_shape=jax.ShapeDtypeStruct((rows, width), BF16),
        name="attention",
        cost_estimate=pl.CostEstimate(flops=4_000_000_000, transcendentals=1_600_000, bytes_accessed=2_000_000),
    )(edge, sink_logit, query_rows, kv, vk)


def ring(shift):
    peers = lax.axis_size("tp")
    return [(i, (i + shift) % peers) for i in range(peers)]


def shift_tp(value, shift):
    return lax.ppermute(value, "tp", ring(shift))


def project_kernel(*refs):
    pieces = (len(refs) - 1) // 2
    out_ref = refs[-1]
    total = dot(refs[0][...], refs[pieces][...])
    for n in range(1, pieces):
        total += dot(refs[n][...], refs[pieces + n][...])
    out_ref[...] = total.astype(BF16)


def project(lefts, rights):
    rows = lefts[0].shape[0]
    width = rights[0].shape[1]
    step = 512
    return pl.pallas_call(
        project_kernel,
        grid=(width // step,),
        in_specs=[pl.BlockSpec(a.shape, lambda i: (0, 0)) for a in lefts]
        + [pl.BlockSpec((b.shape[0], step), lambda i: (0, i)) for b in rights],
        out_specs=pl.BlockSpec((rows, step), lambda i: (0, i)),
        out_shape=jax.ShapeDtypeStruct((rows, width), BF16),
        name="project",
        cost_estimate=pl.CostEstimate(flops=1_100_000_000, transcendentals=0, bytes_accessed=6_000_000),
    )(*lefts, *rights)


def fetch_weight(out_weight):
    peers = lax.axis_size("ep")
    half = out_weight.shape[0] // 2
    core = lax.axis_index("ep") % 2
    mine = lax.dynamic_slice_in_dim(out_weight, core * half, half, 0)
    swap = [(i, i ^ 1) for i in range(peers)]
    fetched = []
    for shift in (1, 3, 2):
        a = shift_tp(mine, shift)
        fetched.append((a, lax.ppermute(a, "ep", swap)))
    return fetched


def mix_tokens(attended, out_weight, fetched):
    peers = lax.axis_size("tp")
    me = lax.axis_index("tp")
    core = lax.axis_index("ep") % 2
    tokens = attended.shape[0] // peers
    half = out_weight.shape[0] // 2

    def block(shift):
        return lax.dynamic_slice_in_dim(attended, (me + shift) % peers * tokens, tokens, 0)

    lefts, rights = [block(0)], [out_weight]
    for shift, (a, b) in zip((1, 3, 2), fetched):
        heads = shift_tp(block(shift), shift)
        lefts.append(lax.dynamic_slice_in_dim(heads, core * half, half, 1))
        lefts.append(lax.dynamic_slice_in_dim(heads, (1 - core) * half, half, 1))
        rights += [a, b]
    return project(lefts, rights)


def expert_kernel(*refs, pieces):
    rows = refs[:pieces]
    gate_ref, up_ref, down_ref = refs[pieces : pieces + 3]
    outs = refs[pieces + 3 : 2 * pieces + 3]
    joined, total = refs[2 * pieces + 3 :]
    step = pl.program_id(0)
    count = rows[0].shape[0]

    @pl.when(step == 0)
    def _():
        for n in range(pieces):
            joined[n * count : (n + 1) * count, :] = rows[n][...]

    x = joined[...]
    gate = dot(x, gate_ref[...])
    up = dot(x, up_ref[...])
    hidden = (gate / (1.0 + jnp.exp(-gate)) * up).astype(BF16)
    part = dot(hidden, down_ref[...])

    @pl.when(step == 0)
    def _():
        total[...] = part

    @pl.when(step > 0)
    def _():
        total[...] += part

    @pl.when(step == pl.num_programs(0) - 1)
    def _():
        for n in range(pieces):
            outs[n][...] = total[n * count : (n + 1) * count, :].astype(BF16)


def expert(rows, gate_weight, up_weight, down_weight):
    pieces = len(rows)
    count, width = rows[0].shape
    units = gate_weight.shape[1]
    step = 256
    whole = pl.BlockSpec((count, width), lambda i: (0, 0))
    columns = pl.BlockSpec((width, step), lambda i: (0, i))
    return pl.pallas_call(
        functools.partial(expert_kernel, pieces=pieces),
        grid=(units // step,),
        in_specs=[whole] * pieces + [columns, columns, pl.BlockSpec((step, width), lambda i: (i, 0))],
        out_specs=[whole] * pieces,
        out_shape=[jax.ShapeDtypeStruct((count, width), BF16)] * pieces,
        scratch_shapes=[
            pltpu.VMEM((pieces * count, width), BF16),
            pltpu.VMEM((pieces * count, width), F32),
        ],
        name="expert",
        cost_estimate=pl.CostEstimate(
            flops=6 * pieces * count * width * units,
            transcendentals=pieces * count * units,
            bytes_accessed=6 * width * units,
        ),
    )(*rows, gate_weight, up_weight, down_weight)


def unpack(packed):
    count = packed.shape[0]
    columns = packed.shape[1] // CAP
    main = packed[:, : columns * MAIN].reshape(count, columns, MAIN, 128)
    main = main.transpose(0, 2, 1, 3).reshape(count * MAIN, columns * 128)
    last = packed[:, columns * MAIN :].reshape(count, columns * 128)
    return jnp.concatenate([main, last], axis=0)


def pack(rows):
    count = rows.shape[0] // CAP
    columns = rows.shape[1] // 128
    main = rows[: count * MAIN].reshape(count, MAIN, columns, 128)
    main = main.transpose(0, 2, 1, 3).reshape(count, columns * MAIN, 128)
    last = rows[count * MAIN :].reshape(count, columns, 128)
    return jnp.concatenate([main, last], axis=1)


def swap_experts(packed):
    return lax.all_to_all(packed, "ep", 0, 0, tiled=True)


def expert_rows(arrived, weights):
    half = arrived.shape[0] // 2
    rows0, rows1 = unpack(arrived[:half]), unpack(arrived[half:])
    right0 = shift_tp(rows0, 1)
    left1 = shift_tp(rows1, 3)
    far0 = shift_tp(right0, 1)
    far1 = shift_tp(left1, 3)
    right1 = shift_tp(rows1, 1)
    left0 = shift_tp(rows0, 3)
    own0, own1 = expert([rows0, rows1], *weights)
    p_right0, p_left1 = expert([right0, left1], *weights)
    p_far0, p_far1 = expert([far0, far1], *weights)
    p_right1, p_left0 = expert([right1, left0], *weights)
    from1_1 = shift_tp(p_left1, 1)
    from3_0 = shift_tp(p_right0, 3)
    via0 = shift_tp(p_far0, 1)
    via1 = shift_tp(p_far1, 3)
    from1_0 = shift_tp((p_left0.astype(F32) + via0.astype(F32)).astype(BF16), 1)
    from3_1 = shift_tp((p_right1.astype(F32) + via1.astype(F32)).astype(BF16), 3)
    low = own0.astype(F32) + from1_0.astype(F32) + from3_0.astype(F32)
    high = own1.astype(F32) + from1_1.astype(F32) + from3_1.astype(F32)
    return jnp.concatenate([pack(low.astype(BF16)), pack(high.astype(BF16))])


def body(
    query_rows,
    key_rows,
    value_rows,
    sink_logit,
    out_weight,
    routed_rows,
    norm_gain,
    routing,
    route_weight,
    gate_weight,
    up_weight,
    down_weight,
):
    experts = lax.axis_size("ep")
    fetched = fetch_weight(out_weight)
    sent = dispatch(routed_rows, norm_gain, routing, route_weight, experts)
    attended = attention(query_rows, key_rows, value_rows, sink_logit)
    mixed = mix_tokens(attended, out_weight, fetched)
    weights = (gate_weight[0], up_weight[0], down_weight[0])
    out, high, low = sent
    arrived = swap_experts(out)
    summed = expert_rows(arrived, weights)
    back = unpack(swap_experts(summed))
    rows = ((0,), (0,))
    return mixed, (dot(high, back, rows) + dot(low, back, rows)).astype(BF16)


def solution(mesh):
    in_specs = (
        P("ep", "tp"),
        P("ep", "tp"),
        P("ep", "tp"),
        P("tp"),
        P("tp", None),
        P(("ep", "tp"), None),
        P(),
        P(("ep", "tp"), None),
        P(("ep", "tp"), None),
        P("ep", None, "tp"),
        P("ep", None, "tp"),
        P("ep", "tp", None),
    )
    out_specs = (P(("ep", "tp"), None), P(("ep", "tp"), None))
    return jax.shard_map(body, mesh=mesh, in_specs=in_specs, out_specs=out_specs, check_vma=False)
```

```python
import functools

import jax
import jax.numpy as jnp
from jax import lax
from jax.experimental import pallas as pl
from jax.experimental.pallas import tpu as pltpu
from jax.sharding import PartitionSpec as P


HEAD_DIM = 64
WINDOW = 128
EPS = 1e-06
CAP = 9
MAIN = 8
F32 = jnp.float32
BF16 = jnp.bfloat16


def dot(a, b, dims=((1,), (0,))):
    return lax.dot_general(a, b, (dims, ((), ())), preferred_element_type=F32)


def slot_iota(shape, experts):
    slot = lax.broadcasted_iota(jnp.int32, shape, 0)
    main = slot < experts * MAIN
    expert_of = jnp.where(main, lax.shift_right_logical(slot, 3), slot - experts * MAIN)
    return expert_of, jnp.where(main, slot & (MAIN - 1), MAIN)


def dispatch_kernel(rows_ref, gain_ref, routing_ref, weight_ref, out_ref, high_ref, low_ref, *, experts):
    tokens, width = rows_ref.shape
    x = rows_ref[...].astype(F32)
    mean = jnp.mean(x * x, axis=-1, keepdims=True)
    normed = (x * lax.rsqrt(mean + EPS) * gain_ref[...]).astype(BF16)
    ids = lax.broadcasted_iota(jnp.int32, (experts, tokens), 0)
    hot0 = routing_ref[0:1, :] == ids
    hot1 = routing_ref[1:2, :] == ids
    member = jnp.where(hot0 | hot1, 1.0, 0.0)
    row = lax.broadcasted_iota(jnp.int32, (tokens, tokens), 0)
    col = lax.broadcasted_iota(jnp.int32, (tokens, tokens), 1)
    upper = jnp.where(row <= col, 1.0, 0.0).astype(BF16)
    place = (dot(member.astype(BF16), upper) * member).astype(BF16)
    gate = jnp.where(hot0, weight_ref[0:1, :], 0.0) + jnp.where(hot1, weight_ref[1:2, :], 0.0)
    high = gate.astype(BF16)
    low = (gate - high.astype(F32)).astype(BF16)
    slots = experts * CAP
    expert_of, _ = slot_iota((slots, experts), experts)
    pick = jnp.where(expert_of == lax.broadcasted_iota(jnp.int32, (slots, experts), 1), 1.0, 0.0)
    pick = pick.astype(BF16)
    _, place_of = slot_iota((slots, tokens), experts)
    here = dot(pick, place) == (place_of + 1).astype(F32)
    high_ref[...] = jnp.where(here, dot(pick, high), 0.0).astype(BF16)
    low_ref[...] = jnp.where(here, dot(pick, low), 0.0).astype(BF16)
    rows = dot(jnp.where(here, 1.0, 0.0).astype(BF16), normed)
    last = []
    for j in range(width // 128):
        part = rows[:, j * 128 : (j + 1) * 128]
        tile = part[: experts * MAIN].reshape(experts, MAIN, 128).astype(BF16)
        out_ref[:, j * MAIN : (j + 1) * MAIN, :] = tile
        last.append(part[experts * MAIN :])
    out_ref[:, width // 128 * MAIN :, :] = jnp.stack(last, axis=1).astype(BF16)


def dispatch(routed_rows, norm_gain, routing, route_weight, experts):
    tokens, width = routed_rows.shape
    slots = experts * CAP
    matrix = jax.ShapeDtypeStruct((slots, tokens), BF16)
    return pl.pallas_call(
        functools.partial(dispatch_kernel, experts=experts),
        out_shape=(jax.ShapeDtypeStruct((experts, CAP * width // 128, 128), BF16), matrix, matrix),
        name="dispatch",
        cost_estimate=pl.CostEstimate(flops=400_000_000, transcendentals=0, bytes_accessed=2_500_000),
    )(routed_rows, norm_gain.reshape(1, width), routing.T, route_weight.T)


def attention_kernel(edge_ref, sink_ref, query_ref, kv_ref, vk_ref, out_ref):
    block = pl.program_id(0)
    size = WINDOW
    start = pl.multiple_of(block * size, size)
    kv = kv_ref[pl.ds(start, 3 * size), :]
    vk = vk_ref[pl.ds(start, 3 * size), :]
    lane = lax.broadcasted_iota(jnp.int32, (3 * size, 2 * HEAD_DIM), 1)
    left = lane < HEAD_DIM
    zero = jnp.zeros_like(kv)
    keys = jnp.concatenate([jnp.where(left, kv, zero), jnp.where(left, zero, vk)], axis=0)
    one = jnp.ones_like(kv)
    values = jnp.concatenate(
        [
            jnp.concatenate([jnp.where(left, vk, zero), jnp.where(left, one, zero)], axis=1),
            jnp.concatenate([jnp.where(left, zero, kv), jnp.where(left, zero, one)], axis=1),
        ],
        axis=0,
    )
    row = lax.broadcasted_iota(jnp.int32, (size, size), 0)
    col = lax.broadcasted_iota(jnp.int32, (size, size), 1)
    off_left = jnp.where((block == 0) & (edge_ref[0] == 1), 4 * size, 0)
    last = pl.num_programs(0) - 1
    off_right = jnp.where((block == last) & (edge_ref[1] == 1), 4 * size, 0)
    keep_left = col >= row + off_left
    keep_right = col + off_right <= row
    for pair in range(query_ref.shape[1] // (2 * HEAD_DIM)):
        lanes = slice(pair * 2 * HEAD_DIM, (pair + 1) * 2 * HEAD_DIM)
        query = query_ref[:, lanes] * jnp.asarray(HEAD_DIM**-0.5, BF16)
        scores = dot(query, keys, ((1,), (1,)))
        weights, sinks = [], []
        for one_head in range(2):
            low = one_head * 3 * size
            s0 = jnp.where(keep_left, scores[:, low : low + size], -jnp.inf)
            s1 = scores[:, low + size : low + 2 * size]
            s2 = jnp.where(keep_right, scores[:, low + 2 * size : low + 3 * size], -jnp.inf)
            sink = sink_ref[2 * pair + one_head]
            peak = jnp.max(jnp.maximum(jnp.maximum(s0, s1), s2), axis=1, keepdims=True)
            peak = jnp.maximum(peak, sink)
            weights += [jnp.exp(s - peak).astype(BF16) for s in (s0, s1, s2)]
            sinks.append(jnp.exp(sink - peak))
        total = dot(jnp.concatenate(weights, axis=1), values)
        lane_q = lax.broadcasted_iota(jnp.int32, (size, 2 * HEAD_DIM), 1)
        denominator = total[:, 2 * HEAD_DIM :] + jnp.where(lane_q < HEAD_DIM, sinks[0], sinks[1])
        out_ref[:, lanes] = (total[:, : 2 * HEAD_DIM] / denominator).astype(BF16)


def halo_rows(key_rows, value_rows):
    peers = lax.axis_size("ep")
    up = [(i, i + 1) for i in range(peers - 1)]
    down = [(j, i) for i, j in up]
    joined = jnp.concatenate([key_rows, value_rows], axis=1)
    rows = joined.shape[0]
    before = lax.ppermute(joined[rows - WINDOW :], "ep", up)
    after = lax.ppermute(joined[:WINDOW], "ep", down)
    return before, joined, after


def attention(query_rows, before, joined, after, sink_logit):
    peers = lax.axis_size("ep")
    me = lax.axis_index("ep")
    rows = joined.shape[0]
    kv = jnp.concatenate([before, joined, after], axis=0)
    vk = jnp.concatenate([kv[:, HEAD_DIM:], kv[:, :HEAD_DIM]], axis=1)
    edge = jnp.stack([me == 0, me == peers - 1]).astype(jnp.int32)
    width = query_rows.shape[1]
    whole = lambda i: (0, 0)
    return pl.pallas_call(
        attention_kernel,
        grid=(rows // WINDOW,),
        in_specs=[
            pl.BlockSpec(memory_space=pltpu.SMEM),
            pl.BlockSpec(memory_space=pltpu.SMEM),
            pl.BlockSpec((WINDOW, width), lambda i: (i, 0)),
            pl.BlockSpec(kv.shape, whole),
            pl.BlockSpec(vk.shape, whole),
        ],
        out_specs=pl.BlockSpec((WINDOW, width), lambda i: (i, 0)),
        out_shape=jax.ShapeDtypeStruct((rows, width), BF16),
        name="attention",
        compiler_params=pltpu.CompilerParams(vmem_limit_bytes=20 * 1024 * 1024),
        cost_estimate=pl.CostEstimate(flops=4_000_000_000, transcendentals=1_600_000, bytes_accessed=2_000_000),
    )(edge, sink_logit, query_rows, kv, vk)


def ring(shift):
    peers = lax.axis_size("tp")
    return [(i, (i + shift) % peers) for i in range(peers)]


def shift_tp(value, shift):
    return lax.ppermute(value, "tp", ring(shift))


def project_kernel(own_ref, right_ref, left_ref, far_ref, weight_ref, fetched_ref, out_ref):
    total = dot(own_ref[...], weight_ref[...])
    for n, heads_ref in enumerate((right_ref, left_ref, far_ref)):
        total += dot(heads_ref[...], fetched_ref[n])
    out_ref[...] = total.astype(BF16)


def project(own, heads, weight, fetched):
    rows = own.shape[0]
    depth, width = weight.shape
    step = 512
    left = pl.BlockSpec((rows, depth), lambda i: (0, 0))
    return pl.pallas_call(
        project_kernel,
        grid=(width // step,),
        in_specs=[left] * 4
        + [
            pl.BlockSpec((depth, step), lambda i: (0, i)),
            pl.BlockSpec((len(heads), depth, step), lambda i: (0, 0, i)),
        ],
        out_specs=pl.BlockSpec((rows, step), lambda i: (0, i)),
        out_shape=jax.ShapeDtypeStruct((rows, width), BF16),
        name="project",
        compiler_params=pltpu.CompilerParams(vmem_limit_bytes=20 * 1024 * 1024),
        cost_estimate=pl.CostEstimate(flops=1_100_000_000, transcendentals=0, bytes_accessed=6_000_000),
    )(own, *heads, weight, fetched)


def fetch_weight(out_weight):
    peers = lax.axis_size("ep")
    me = lax.axis_index("ep")
    quarter = me % 4
    rows = out_weight.shape[0] // 4
    mine = lax.dynamic_slice_in_dim(out_weight, quarter * rows, rows, 0)
    fetched = []
    for shift in (1, 3, 2):
        fetched.append(shift_tp(mine, shift))
    first = jnp.stack(fetched)
    second = lax.ppermute(first, "ep", [(i, i ^ 2) for i in range(peers)])
    third = lax.ppermute(first, "ep", [(i, i ^ 1) for i in range(peers)])
    fourth = lax.ppermute(second, "ep", [(i, i ^ 1) for i in range(peers)])
    return first, third, second, fourth


def join_weight(pieces):
    count, rows, width = pieces[0].shape
    quarter = lax.axis_index("ep") % 4
    whole = jnp.zeros((count, 4, rows, width), BF16)
    for n, piece in enumerate(pieces):
        whole = lax.dynamic_update_slice_in_dim(whole, piece[:, None], quarter ^ n, 1)
    return whole.reshape(count, 4 * rows, width)


def mix_tokens(attended, out_weight, fetched):
    peers = lax.axis_size("tp")
    me = lax.axis_index("tp")
    tokens = attended.shape[0] // peers

    def block(shift):
        return lax.dynamic_slice_in_dim(attended, (me + shift) % peers * tokens, tokens, 0)

    heads = []
    for shift in (1, 3, 2):
        heads.append(shift_tp(block(shift), shift))
    return project(block(0), heads, out_weight, join_weight(fetched))


def unpack_into(out_ref, base, packed_ref):
    count = packed_ref.shape[0]
    columns = packed_ref.shape[1] // CAP
    last = packed_ref[:, columns * MAIN :, :].astype(F32)
    for j in range(columns):
        lanes = slice(j * 128, (j + 1) * 128)
        tile = packed_ref[:, j * MAIN : (j + 1) * MAIN, :].astype(F32)
        out_ref[base : base + count * MAIN, lanes] = tile.reshape(count * MAIN, 128).astype(BF16)
        out_ref[base + count * MAIN : base + count * CAP, lanes] = last[:, j, :].astype(BF16)


def expert_kernel(*refs, pieces, step, columns):
    rows = refs[:pieces]
    gate_hbm, up_hbm, down_hbm = refs[pieces : pieces + 3]
    outs = refs[pieces + 3 : 2 * pieces + 3]
    joined, hidden, gate, up, down, gate_sem, up_sem, down_sem = refs[2 * pieces + 3 :]
    count = joined.shape[0] // pieces

    def part(source, target, sems, k, size):
        lanes = pl.ds(pl.multiple_of(k * size, size), size)
        return pltpu.make_async_copy(source.at[:, lanes], target.at[k], sems.at[k])

    for k in range(gate.shape[0]):
        part(gate_hbm, gate, gate_sem, k, step).start()
        part(up_hbm, up, up_sem, k, step).start()
    for k in range(down.shape[0]):
        part(down_hbm, down, down_sem, k, columns).start()
    for n in range(pieces):
        unpack_into(joined, n * count, rows[n])

    def first(k, carry):
        part(gate_hbm, gate, gate_sem, k, step).wait()
        part(up_hbm, up, up_sem, k, step).wait()
        x = joined[...]
        g = dot(x, gate[k])
        hidden[k] = (g / (1.0 + jnp.exp(-g)) * dot(x, up[k])).astype(BF16)
        return carry

    lax.fori_loop(0, gate.shape[0], first, 0)

    def second(k, carry):
        part(down_hbm, down, down_sem, k, columns).wait()
        h = jnp.concatenate([hidden[n] for n in range(hidden.shape[0])], axis=1)
        out = dot(h, down[k]).astype(BF16)
        lanes = pl.ds(pl.multiple_of(k * columns, columns), columns)
        for n in range(pieces):
            outs[n][:, lanes] = out[n * count : (n + 1) * count]
        return carry

    lax.fori_loop(0, down.shape[0], second, 0)


def expert(rows, gate_weight, up_weight, down_weight):
    pieces = len(rows)
    width, units = gate_weight.shape
    count = rows[0].shape[0] * CAP
    step, columns = 256, 1024
    vmem = pl.BlockSpec(memory_space=pltpu.VMEM)
    hbm = pl.BlockSpec(memory_space=pl.ANY)
    return pl.pallas_call(
        functools.partial(expert_kernel, pieces=pieces, step=step, columns=columns),
        in_specs=[vmem] * pieces + [hbm] * 3,
        out_specs=[vmem] * pieces,
        out_shape=[jax.ShapeDtypeStruct((count, width), BF16)] * pieces,
        scratch_shapes=[
            pltpu.VMEM((pieces * count, width), BF16),
            pltpu.VMEM((units // step, pieces * count, step), BF16),
            pltpu.VMEM((units // step, width, step), BF16),
            pltpu.VMEM((units // step, width, step), BF16),
            pltpu.VMEM((width // columns, units, columns), BF16),
            pltpu.SemaphoreType.DMA((units // step,)),
            pltpu.SemaphoreType.DMA((units // step,)),
            pltpu.SemaphoreType.DMA((width // columns,)),
        ],
        name="expert",
        compiler_params=pltpu.CompilerParams(vmem_limit_bytes=36 * 1024 * 1024),
        cost_estimate=pl.CostEstimate(
            flops=6 * pieces * count * width * units,
            transcendentals=pieces * count * units,
            bytes_accessed=6 * width * units,
        ),
    )(*rows, gate_weight, up_weight, down_weight)


def combine_kernel(packed_ref, high_ref, low_ref, out_ref, rows):
    unpack_into(rows, 0, packed_ref)
    back = rows[...]
    slots = ((0,), (0,))
    out_ref[...] = (dot(high_ref[...], back, slots) + dot(low_ref[...], back, slots)).astype(BF16)


def combine(packed, high, low):
    slots, tokens = high.shape
    width = packed.shape[1] // CAP * 128
    return pl.pallas_call(
        combine_kernel,
        out_shape=jax.ShapeDtypeStruct((tokens, width), BF16),
        scratch_shapes=[pltpu.VMEM((slots, width), BF16)],
        name="combine",
        compiler_params=pltpu.CompilerParams(vmem_limit_bytes=20 * 1024 * 1024),
        cost_estimate=pl.CostEstimate(flops=300_000_000, transcendentals=0, bytes_accessed=2_000_000),
    )(packed, high, low)


def sum_kernel(*refs):
    out_ref = refs[-1]
    for half in range(2):
        parts = refs[3 * half : 3 * half + 3]
        rows = parts[0][...].astype(F32) + parts[1][...].astype(F32) + parts[2][...].astype(F32)
        count = rows.shape[0] // CAP
        columns = rows.shape[1] // 128
        here = slice(half * count, (half + 1) * count)
        last = []
        for j in range(columns):
            piece = rows[:, j * 128 : (j + 1) * 128]
            tile = piece[: count * MAIN].reshape(count, MAIN, 128).astype(BF16)
            out_ref[here, j * MAIN : (j + 1) * MAIN, :] = tile
            last.append(piece[count * MAIN :])
        out_ref[here, columns * MAIN :, :] = jnp.stack(last, axis=1).astype(BF16)


def sum_rows(low, high):
    count, width = low[0].shape
    return pl.pallas_call(
        sum_kernel,
        out_shape=jax.ShapeDtypeStruct((2 * count // CAP, CAP * width // 128, 128), BF16),
        name="sum_rows",
        compiler_params=pltpu.CompilerParams(vmem_limit_bytes=20 * 1024 * 1024),
        cost_estimate=pl.CostEstimate(flops=2_000_000, transcendentals=0, bytes_accessed=5_000_000),
    )(*low, *high)


def swap_experts(packed):
    return lax.all_to_all(packed, "ep", 0, 0, tiled=True)


def expert_rows(arrived, weights):
    half = arrived.shape[0] // 2
    rows0, rows1 = arrived[:half], arrived[half:]
    right0 = shift_tp(rows0, 1)
    left1 = shift_tp(rows1, 3)
    far0 = shift_tp(right0, 1)
    far1 = shift_tp(left1, 3)
    right1 = shift_tp(rows1, 1)
    left0 = shift_tp(rows0, 3)
    own0, own1 = expert([rows0, rows1], *weights)
    p_right0, p_left1 = expert([right0, left1], *weights)
    p_far0, p_far1 = expert([far0, far1], *weights)
    p_right1, p_left0 = expert([right1, left0], *weights)
    from1_1 = shift_tp(p_left1, 1)
    from3_0 = shift_tp(p_right0, 3)
    via0 = shift_tp(p_far0, 1)
    via1 = shift_tp(p_far1, 3)
    from1_0 = shift_tp((p_left0.astype(F32) + via0.astype(F32)).astype(BF16), 1)
    from3_1 = shift_tp((p_right1.astype(F32) + via1.astype(F32)).astype(BF16), 3)
    return sum_rows((own0, from1_0, from3_0), (own1, from1_1, from3_1)), p_right0, p_right1


def body(
    query_rows,
    key_rows,
    value_rows,
    sink_logit,
    out_weight,
    routed_rows,
    norm_gain,
    routing,
    route_weight,
    gate_weight,
    up_weight,
    down_weight,
):
    experts = lax.axis_size("ep")
    fetched = fetch_weight(out_weight)
    sent = dispatch(routed_rows, norm_gain, routing, route_weight, experts)
    halo = halo_rows(key_rows, value_rows)
    weights = (gate_weight[0], up_weight[0], down_weight[0])
    out, high, low = sent
    arrived = swap_experts(out)
    summed, early, late = expert_rows(arrived, weights)
    before, joined, after, _ = lax.optimization_barrier((*halo, early))
    fetched, _ = lax.optimization_barrier((fetched, late))
    attended = attention(query_rows, before, joined, after, sink_logit)
    mixed = mix_tokens(attended, out_weight, fetched)
    back = swap_experts(summed)
    return mixed, combine(back, high, low)


def solution(mesh):
    in_specs = (
        P("ep", "tp"),
        P("ep", "tp"),
        P("ep", "tp"),
        P("tp"),
        P("tp", None),
        P(("ep", "tp"), None),
        P(),
        P(("ep", "tp"), None),
        P(("ep", "tp"), None),
        P("ep", None, "tp"),
        P("ep", None, "tp"),
        P("ep", "tp", None),
    )
    out_specs = (P(("ep", "tp"), None), P(("ep", "tp"), None))
    return jax.shard_map(body, mesh=mesh, in_specs=in_specs, out_specs=out_specs, check_vma=False)
```
